256 devices in a mesh: fs: 16 (over y, x), tp: 16 (over z, core).
Axes of the slice: x: 4, y: 4, z: 8, core: 2. Of those that a mesh axis runs over, the one named last changes fastest.
Arguments:
- tokens: bfloat16 [32768, 2048], P(('fs', 'tp')), may hold values from -6 to 6
- up_weight: bfloat16 [2048, 4096], P('fs', 'tp'), may hold values from -0.125 to 0.125
- down_weight: bfloat16 [4096, 2048], P('tp', 'fs'), may hold values from -0.09375 to 0.09375
- cotangent: bfloat16 [32768, 2048], P(('fs', 'tp')), may hold values from -24 to 24
Outputs:
- input_grad: bfloat16 [32768, 2048], P(('fs', 'tp'))
- up_grad: float32 [2048, 4096], P('fs', 'tp')
- down_grad: float32 [4096, 2048], P('tp', 'fs')
The draws below stay inside these ranges and needn't reach their ends.
All inputs are finite; a program needn't handle non-finite values.
Results may differ from the reference program's by a relative error of at most 0.018.
Values may be sent and summed in bfloat16 or wider, within the bound.
No kernel may reach another device: no remote copies, remote signals or barrier semaphores. Data moves between devices by JAX's collectives and lax.ppermute only.
A program may use at most 128 MiB of HBM per device.

```python
import jax
import jax.numpy as jnp
from jax import lax

D = 2048
FF = 4096
TOKENS = 32768
N_TP = 16


def spiked(entries, own_key, source, target, blocks, factor):
    owner, partner = [(jnp.arange(entries.shape[dim]) // (entries.shape[dim] // blocks)).reshape([-1 if axis == dim else 1 for axis in range(entries.ndim)]) for dim in (source, target)]
    chosen = jax.random.permutation(own_key, blocks)[partner]
    strong = (owner == chosen) | (owner == (partner + blocks // 2) % blocks)
    return jnp.where(strong, factor * entries, entries)


def levels(own_key, dims, pieces, low, high):
    loudness = 1.0
    for axis_at, parts in pieces:
        heights = jax.random.uniform(jax.random.fold_in(jax.random.fold_in(own_key, 6), axis_at), (parts,), jnp.float32, low / len(pieces), high / len(pieces))
        loudness = loudness * jnp.repeat(jnp.exp(heights), dims[axis_at] // parts).reshape((-1,) + (1,) * (len(dims) - 1 - axis_at))
    return loudness


def bell_draw(key, shape, spread, reach, split=(), kind=jnp.bfloat16):
    level = levels(key, shape, split, -0.22, 0.18) if split else 1.0
    drawn = jax.random.normal(key, shape, jnp.float32) * spread * level
    return jnp.minimum(jnp.maximum(drawn, -reach), reach).astype(kind)


def gaussian_with(rng, dims, spread, bound, pieces, heavy, held_as=jnp.bfloat16):
    values = spread * jax.random.normal(rng, dims, jnp.float32)
    if pieces:
        values = values * levels(rng, dims, pieces, -0.22, 0.18)
    return jnp.clip(spiked(values, jax.random.fold_in(rng, 3), *heavy), -bound, bound).astype(held_as)


def setup_inputs(seed: int = 0) -> dict:
    key_list = jax.random.split(jax.random.key(seed), 5)
    return {
        "tokens": bell_draw(key_list[0], (TOKENS, D), 1.0, 6.0, ((0, 256),)),
        "up_weight": bell_draw(key_list[1], (D, FF), D ** -0.5, 0.125, ((0, 16), (1, 16))),
        "down_weight": bell_draw(key_list[2], (FF, D), FF ** -0.5, 0.09375, ((0, 16), (1, 16))),
        "cotangent": gaussian_with(key_list[3], (TOKENS, D), 1.0, 24.0, ((0, 256),), (0, 1, 256, 6.0)),
    }


def reference(tokens, up_weight, down_weight, cotangent):
    pre = jnp.dot(tokens, up_weight, preferred_element_type=jnp.float32)
    active = jnp.maximum(pre, 0.0)
    hidden = (active * active).astype(jnp.bfloat16)
    dhidden = jnp.dot(cotangent, down_weight.T, preferred_element_type=jnp.float32)
    dpre = (2.0 * active * dhidden).astype(jnp.bfloat16)
    factor = 1.0 / jnp.sqrt(jnp.float32(TOKENS))
    down_grad = jnp.dot(hidden.T, cotangent, preferred_element_type=jnp.float32) * factor
    up_grad = jnp.dot(tokens.T, dpre, preferred_element_type=jnp.float32) * factor
    width = FF // N_TP

    def add_block(index, total):
        start = (index * width).astype(jnp.int32)
        cols = lax.dynamic_slice_in_dim(dpre, start, width, 1)
        right = lax.dynamic_slice_in_dim(up_weight, start, width, 1)
        part = jnp.dot(cols, right.T, preferred_element_type=jnp.float32).astype(jnp.bfloat16)
        part = lax.optimization_barrier(part)
        return total + part.astype(jnp.float32)
    total = lax.fori_loop(jnp.int32(0), jnp.int32(N_TP), add_block, jnp.zeros((TOKENS, D), jnp.float32))
    return (total.astype(jnp.bfloat16), up_grad, down_grad)
```

```python
import jax
import jax.numpy as jnp
from jax import lax
from jax.experimental import pallas as pl
from jax.experimental.pallas import tpu as pltpu
from jax.sharding import Mesh, PartitionSpec as P


F32, BF16 = jnp.float32, jnp.bfloat16
NX, NY, NZ = 4, 4, 8
ROWS, D, CUT, LANES, HID = 128, 2048, 64, 128, 512
TOKENS = 32768
NN = (((1,), (0,)), ((), ()))
NT = (((1,), (1,)), ((), ()))


def call(body, outs, n_in, scratch=(), flops=0):
    spec = pl.BlockSpec(memory_space=pltpu.VMEM)
    return pl.pallas_call(
        body,
        out_shape=[jax.ShapeDtypeStruct(s, d) for s, d in outs],
        in_specs=[spec] * n_in,
        out_specs=[spec] * len(outs),
        scratch_shapes=[pltpu.VMEM(s, d) for s, d in scratch],
        compiler_params=pltpu.CompilerParams(vmem_limit_bytes=56 * 2**20),
        cost_estimate=pl.CostEstimate(flops=flops, bytes_accessed=0, transcendentals=0),
    )


def cut_weights(up, down, o0, o1, o2, o3, turned):
    x = lax.axis_index("x")
    turned[...] = up[...].astype(F32).T.astype(BF16)
    for s, out in enumerate((o0, o1, o2, o3)):
        at = pl.ds(pl.multiple_of(lax.rem(x + s, NX) * CUT, CUT), CUT)
        out[0] = turned[at, :]
        out[1] = down[at, :]


def column(x, y, k, s, width=LANES):
    block = lax.rem(y + NY - k, NY) * NX + lax.rem(x + NX - s, NX)
    return pl.ds(pl.multiple_of(block * LANES, LANES), width)


def first(*refs):
    ups, downs = refs[:9], refs[9:14]
    fulls, halves = refs[14:20], refs[20:24]
    outs = refs[24:]
    tok_o, up_o, dpre_o, dpre_t = outs[:4]
    down_out = outs[4:9]
    cot_v, down_v, hid_t = outs[9:]
    x, y = lax.axis_index("x"), lax.axis_index("y")
    for z in range(NZ):
        for k in range(NY):
            for s in range(NX):
                at = column(x, y, k, s)
                row = pl.ds(z * CUT, CUT)
                if z < 7:
                    up_o[row, at] = ups[z][k, s]
                else:
                    up_o[row, at] = ups[7 + k // 2][k % 2, s]
                if k == 2:
                    down_v[row, at] = downs[2 + z // 4][z % 4, s]
                else:
                    down_v[row, at] = downs[{0: 0, 1: 1, 3: 4}[k]][z, s]
    for at, piece in enumerate(fulls):
        block = {0: 0, 1: 4, 2: 1, 3: 5, 4: 2, 5: 6}[at]
        for h in range(2):
            row = pl.ds(block * ROWS + h * 64, 64)
            tok_o[row, :] = piece[h, 0]
            cot_v[row, :] = piece[h, 1]
    for at, piece in enumerate(halves):
        row = pl.ds((3 + 4 * (at // 2)) * ROWS + (at % 2) * 64, 64)
        tok_o[row, :] = piece[0]
        cot_v[row, :] = piece[1]
    for i in range(4):
        row = pl.ds(i * 256, 256)
        pre = lax.dot_general(tok_o[row, :], up_o[...], NT, preferred_element_type=F32)
        act = jnp.maximum(pre, 0.0)
        hidden = (act * act).astype(BF16)
        hid_t[:, row] = hidden.T
        dhid = lax.dot_general(cot_v[row, :], down_v[...], NT, preferred_element_type=F32)
        dpre = (2.0 * act * dhid).astype(BF16)
        dpre_o[row, :] = dpre
        dpre_t[:, row] = dpre.T
    for j in range(NY):
        at = pl.ds(pl.multiple_of(lax.rem(y + j, NY) * 512, 512), 512)
        term = lax.dot_general(hid_t[...], cot_v[:, at], NN, preferred_element_type=F32).astype(BF16)
        for block in range(NX):
            s = lax.rem(block + NX - x, NX)
            part = term[:, block * LANES : (block + 1) * LANES].reshape(NZ, CUT, LANES)
            if j == 2:
                down_out[2][:, s] = part[:4]
                down_out[3][:, s] = part[4:]
            else:
                down_out[{0: 0, 1: 1, 3: 4}[j]][:, s] = part


def second(dpre_t, tok, *outs):
    x, y = lax.axis_index("x"), lax.axis_index("y")
    for j in range(NY):
        at = pl.ds(pl.multiple_of(lax.rem(y + j, NY) * 512, 512), 512)
        term = lax.dot_general(dpre_t[...], tok[:, at], NN, preferred_element_type=F32).astype(BF16)
        for block in range(NX):
            s = lax.rem(block + NX - x, NX)
            part = term[:, block * LANES : (block + 1) * LANES]
            for z in range(NZ):
                piece = part[z * CUT : (z + 1) * CUT]
                if z < 7:
                    outs[z][j, s] = piece
                else:
                    outs[7 + j // 2][j % 2, s] = piece


def third(half):
    def body(dpre, up, out):
        for i in range(2):
            row = pl.ds(half * 512 + i * 256, 256)
            out[pl.ds(i * 256, 256), :] = lax.dot_general(
                dpre[row, :], up[...], NN, preferred_element_type=F32
            ).astype(BF16)

    return body


def last(r0, r1, r2, r3, up_out, down_out, turned):
    x = lax.axis_index("x")
    factor = 1.0 / jnp.sqrt(jnp.float32(TOKENS))
    for s, ref in enumerate((r0, r1, r2, r3)):
        at = pl.ds(pl.multiple_of(lax.rem(x + NX - s, NX) * CUT, CUT), CUT)
        turned[at, :] = ref[0].astype(F32) * factor
        down_out[at, :] = ref[1].astype(F32) * factor
    up_out[...] = turned[...].T


def shift(value, axis, by):
    n = lax.axis_size(axis)
    return lax.ppermute(value, axis, [(i, (i + by) % n) for i in range(n)])


def add(*values):
    total = values[0].astype(F32)
    for v in values[1:]:
        total = total + v.astype(F32)
    return total.astype(BF16)


def shards(tokens, up_weight, down_weight, cotangent):
    w = call(cut_weights, [((2, CUT, LANES), BF16)] * 4, 2, [((256, LANES), BF16)])(up_weight, down_weight)
    w = [w[0]] + [shift(w[s], "x", s) for s in (1, 2, 3)]
    own = jnp.stack([tokens.reshape(2, 64, D), cotangent.reshape(2, 64, D)], axis=1)
    left, right = shift(own, "x", 1), shift(own, "x", -1)
    mate = shift(own, "core", 1)

    u0 = jnp.stack([v[0] for v in w])
    d0 = jnp.stack([v[1] for v in w])
    u1, u3, u2 = shift(u0, "y", 1), shift(u0, "y", -1), shift(u0, "y", 2)
    ds = [d0] + [shift(d0, "z", b) for b in (1, 2, 3, -1, -2, -3, 4)]
    uz = jnp.stack([u0, u1, u2, u3])
    m1, p1 = shift(uz, "z", 1), shift(uz, "z", -1)
    dz = jnp.stack(ds)
    dy1, dy3 = shift(dz, "y", 1), shift(dz, "y", -1)
    m2, p2 = shift(m1, "z", 1), shift(p1, "z", -1)
    far_a, far_b = shift(left[0], "x", 1), shift(right[1], "x", -1)
    left_m, right_m = shift(left, "core", 1), shift(right, "core", 1)
    m3, p3 = shift(m2, "z", 1), shift(p2, "z", -1)
    dy2a, dy2b = shift(dy1[:4], "y", 1), shift(dy3[4:], "y", -1)
    opp_a, opp_b = shift(m3[:2], "z", 1), shift(p3[2:], "z", -1)
    far_am, far_bm = shift(far_a, "core", 1), shift(far_b, "core", 1)

    one = 2 * 1024 * D * HID
    piece = ((NZ, NX, CUT, LANES), BF16)
    half = ((4, NX, CUT, LANES), BF16)
    tok, up, dpre, dpre_t, g0, g1, g2a, g2b, g3 = call(
        first,
        [((1024, D), BF16), ((HID, D), BF16), ((1024, HID), BF16), ((HID, 1024), BF16), piece, piece, half, half, piece],
        24,
        [((1024, D), BF16), ((HID, D), BF16), ((HID, 1024), BF16)],
        3 * one,
    )(uz, m1, m2, m3, p1, p2, p3, opp_a, opp_b, dz, dy1, dy2a, dy2b, dy3,
      own, mate, left, left_m, right, right_m, far_a, far_b, far_am, far_bm)

    ga, gb = shift(g2a, "y", 1), shift(g2b, "y", -1)
    piece = ((NY, NX, CUT, LANES), BF16)
    half = ((2, NX, CUT, LANES), BF16)
    h0, hm1, hm2, hm3, hp1, hp2, hp3, ha, hb = call(second, [piece] * 7 + [half] * 2, 2, (), one)(dpre_t, tok)
    ra, rb = shift(ha, "z", 1), shift(hb, "z", -1)
    ga = shift(jnp.concatenate([add(g1[:4], ga), g1[4:]]), "y", 1)
    gb = shift(jnp.concatenate([g3[:4], add(g3[4:], gb)]), "y", -1)
    (out_m,) = call(third(1), [((512, D), BF16)], 2, (), one // 2)(dpre, up)
    got = shift(out_m, "core", 1)
    (out_o,) = call(third(0), [((512, D), BF16)], 2, (), one // 2)(dpre, up)
    ra = shift(jnp.concatenate([add(hp3[:2], ra), hp3[2:]]), "z", 1)
    rb = shift(jnp.concatenate([hm3[:2], add(hm3[2:], rb)]), "z", -1)
    o = [(out_o[i * ROWS : (i + 1) * ROWS], got[i * ROWS : (i + 1) * ROWS]) for i in range(4)]
    xa = shift(add(o[3][0][:64], o[3][1][:64]), "x", 1)
    xb = shift(add(o[3][0][64:], o[3][1][64:]), "x", -1)
    g = add(g0, ga, gb)
    gs = [g[0]] + [shift(g[i], "z", -b) for i, b in zip(range(1, 8), (1, 2, 3, -1, -2, -3, 4))]
    ra, rb = shift(add(hp2, ra), "z", 1), shift(add(hm2, rb), "z", -1)
    xr = shift(jnp.concatenate([add(o[2][0][:64], o[2][1][:64], xa), add(o[2][0][64:], o[2][1][64:])]), "x", 1)
    xl = shift(jnp.concatenate([add(o[1][0][:64], o[1][1][:64]), add(o[1][0][64:], o[1][1][64:], xb)]), "x", -1)
    ra, rb = shift(add(hp1, ra), "z", 1), shift(add(hm1, rb), "z", -1)
    down_sum = add(*gs)
    h = add(h0, ra, rb)
    hs = [h[0], shift(h[1], "y", 1), shift(h[2], "y", 2), shift(h[3], "y", -1)]
    input_grad = add(o[0][0], o[0][1], xr, xl)
    both = jnp.stack([add(*hs), down_sum], axis=1)
    fin = [both[0]] + [shift(both[s], "x", s) for s in (1, 2, 3)]
    up_grad, down_grad = call(
        last, [((ROWS, 256), F32), ((256, LANES), F32)], 4, [((256, LANES), F32)]
    )(*fin)
    return input_grad, up_grad, down_grad


def solution(mesh):
    fine = Mesh(mesh.devices.reshape(NY, NX, NZ, 2), ("y", "x", "z", "core"))
    rows = P(("y", "x", "z", "core"), None)
    up_spec = P(("y", "x"), ("z", "core"))
    down_spec = P(("z", "core"), ("y", "x"))
    return jax.shard_map(
        shards,
        mesh=fine,
        in_specs=(rows, up_spec, down_spec, rows),
        out_specs=(rows, up_spec, down_spec),
        check_vma=False,
    )
```
